512 devices in a mesh: grp: 2 (over y), sp: 32 (over z), dp: 8 (over x, core).
Axes of the slice: x: 4, y: 2, z: 32, core: 2. Of those that a mesh axis runs over, the one named last changes fastest.
The devices are a block of a 4x8x32 slice.
Arguments:
- tokens: bfloat16 [16, 12288, 2048], P(('grp', 'dp'), 'sp'), parts along dimension 0, may hold values from -6 to 6
- w_value: bfloat16 [2048, 1024], P('dp', 'sp'), may hold values from -0.125 to 0.125
- w_gate: bfloat16 [2048, 1024], P('dp', 'sp'), may hold values from -0.125 to 0.125
- conv_weight: bfloat16 [31, 1024], replicated, may hold values from -20 to 20
- norm_gain: float32 [1024], replicated, may hold values from 0.1 to 1.9
- norm_bias: float32 [1024], replicated, may hold values from -3 to 3
- w_out: bfloat16 [1024, 2048], P('sp', 'dp'), may hold values from -0.1875 to 0.1875
Outputs:
- mixed: bfloat16 [16, 12288, 2048], P(('grp', 'dp'), 'sp'), parts along dimension 0
The draws below stay inside these ranges and needn't reach their ends.
There are 2 independent parts, one for each index of `grp`. The reference program is written for one: setup_inputs(seed, part) draws one part's arguments, and reference() takes and returns one part's arrays. A program takes and returns all parts, laid end to end along the dimension named above; an argument that names none is the same for every part. Nothing has to cross between parts.
All inputs are finite; a program needn't handle non-finite values.
Results may differ from the reference program's by a relative error of at most 0.012.
Values may be sent and summed in bfloat16 or wider, within the bound.
No kernel may reach another device: no remote copies, remote signals or barrier semaphores. Data moves between devices by JAX's collectives and lax.ppermute only.
A program may use at most 64 MiB of HBM per device.

```python
import math
import jax
import jax.numpy as jnp
from jax import lax

D = 2048
C = 1024
KERNEL = 31
SEQ = 12288
SEQS = 8


def draw_conv_weight(key, part):
    first, second = jax.random.split(jax.random.fold_in(key, 11))
    ramp = jnp.arange(C, dtype=jnp.float32) / C
    base = jnp.clip(jax.random.normal(first, (KERNEL, C), jnp.float32), -4.0, 4.0)
    rising = jnp.exp(ramp * math.log(4.0))
    rough = jnp.exp(jax.random.uniform(second, (C,), jnp.float32, -0.7, 0.7))
    return (base * rising * rough / math.sqrt(KERNEL)).astype(jnp.bfloat16)


def block_levels(key, shape, shards, smallest, largest):
    loudness = 1.0
    for position, blocks in shards:
        heights = jax.random.uniform(jax.random.fold_in(jax.random.fold_in(key, 6), position), (blocks,), jnp.float32, smallest / len(shards), largest / len(shards))
        loudness = loudness * jnp.repeat(jnp.exp(heights), shape[position] // blocks).reshape((-1,) + (1,) * (len(shape) - 1 - position))
    return loudness


def bell_draw(rng, dims, scale, reach, cuts=(), kind=jnp.bfloat16):
    drawn = scale * jax.random.normal(rng, dims, jnp.float32)
    if cuts:
        drawn = drawn * block_levels(rng, dims, cuts, -0.22, 0.18)
    return jnp.clip(drawn, -reach, reach).astype(kind)


def setup_inputs(seed: int = 0, part: int = 0) -> dict:
    splits = jax.random.split(jax.random.key(seed), 8)
    part_splits = jax.random.split(jax.random.fold_in(splits[7], part), 8)
    return {
        "tokens": bell_draw(part_splits[0], (SEQS, SEQ, D), 1.0, 6.0, ((0, 8), (1, 32))),
        "w_value": bell_draw(splits[1], (D, C), D ** -0.5, 0.125, ((0, 8), (1, 32))),
        "w_gate": bell_draw(splits[2], (D, C), D ** -0.5, 0.125, ((0, 8), (1, 32))),
        "conv_weight": draw_conv_weight(jax.random.fold_in(splits[7], 71), part),
        "norm_gain": jnp.clip(1.0 + 0.18 * jax.random.normal(splits[4], (C,), jnp.float32), 0.1, 1.9),
        "norm_bias": bell_draw(splits[5], (C,), 0.5, 3.0, (), jnp.float32),
        "w_out": bell_draw(splits[6], (C, D), C ** -0.5, 0.1875, ((0, 32), (1, 8))),
    }


EPS = 1e-05

def one_sequence(seq_rows, w_value, w_gate, conv_weight, norm_gain, norm_bias, w_out):
    value = jnp.dot(seq_rows, w_value, preferred_element_type=jnp.float32)
    gate = jnp.dot(seq_rows, w_gate, preferred_element_type=jnp.float32)
    glu = (value * jax.nn.sigmoid(gate)).astype(jnp.bfloat16)
    length = glu.shape[0]
    glu_f = glu.astype(jnp.float32)
    padded = jnp.concatenate([jnp.zeros((KERNEL - 1, glu.shape[1]), jnp.float32), glu_f], axis=0)
    taps = conv_weight.astype(jnp.float32)
    total = jnp.zeros((length, glu.shape[1]), jnp.float32)
    for tap in range(KERNEL):
        begin = KERNEL - 1 - tap
        total = total + taps[tap][None, :] * padded[begin:begin + length]
    conv = total.astype(jnp.bfloat16)
    conv_f = conv.astype(jnp.float32)
    mean = lax.optimization_barrier(jnp.mean(conv_f, axis=1, keepdims=True))
    meansq = lax.optimization_barrier(jnp.mean(conv_f * conv_f, axis=1, keepdims=True))
    scaled = (conv_f - mean) * lax.rsqrt(meansq - mean * mean + EPS) * norm_gain + norm_bias
    normed = jax.nn.silu(scaled).astype(jnp.bfloat16)
    return jnp.dot(normed, w_out, preferred_element_type=jnp.float32).astype(jnp.bfloat16)

def reference(tokens, w_value, w_gate, conv_weight, norm_gain, norm_bias, w_out):
    return lax.map(lambda seq_rows: one_sequence(seq_rows, w_value, w_gate, conv_weight, norm_gain, norm_bias, w_out), tokens)
```

```python
import jax
import jax.numpy as jnp
from jax import lax
from jax.experimental import pallas as pl
from jax.experimental.pallas import tpu as pltpu
from jax.sharding import Mesh, PartitionSpec as P

EPS = 1e-05
HALO = 32
PIECE = 256
LANES = 128


def spread(block, axis):
    members = lax.axis_size(axis)
    return lax.all_to_all(jnp.broadcast_to(block, (members, *block.shape)), axis, 0, 0)


def swapped(array, axis):
    return lax.ppermute(array, axis, [(0, 1), (1, 0)])


def body(
    where_ref, halo_ref, tok_ref, cw_ref, gain_ref, bias_ref,
    vg0_ref, vg1_ref, oa0_ref, ob0_ref, oa1_ref, ob1_ref, out_ref,
    tok, w, shifted, conv, sums, squares, tok_sem, vg_sem, o_sem,
):
    core, side = where_ref[0], where_ref[1]
    rows = out_ref.shape[0]
    taps = cw_ref.shape[0]
    blocks = vg0_ref.shape[0]
    copies = [
        pltpu.make_async_copy(halo_ref, tok.at[pl.ds(0, HALO)], tok_sem.at[0]),
        pltpu.make_async_copy(tok_ref, tok.at[pl.ds(HALO, rows)], tok_sem.at[1]),
    ]
    late = []
    at = 0
    for mine, vg in enumerate((vg0_ref, vg1_ref)):
        c = core if mine == 0 else 1 - core
        for x in range(blocks):
            for other in range(2):
                s = side if other == 0 else 1 - side
                for m in range(2):
                    copies.append(pltpu.make_async_copy(vg.at[x, other, m], w.at[m, 2 * x + c, :, s], vg_sem.at[at]))
                    at += 1
    at = 0
    for mine, pair in enumerate(((oa0_ref, ob0_ref), (oa1_ref, ob1_ref))):
        c = core if mine == 0 else 1 - core
        for other, o in enumerate(pair):
            s = side if other == 0 else 1 - side
            for x in range(blocks):
                late.append(pltpu.make_async_copy(o.at[x], w.at[2, 2 * x + c, :, s], o_sem.at[at]))
                at += 1
    for c in copies:
        c.start()
    for c in late:
        c.start()
    for c in copies:
        c.wait()

    ks = w.shape[1]
    channels = cw_ref.shape[1]
    zs = PIECE // 32
    length = rows + HALO
    for q in range(channels // PIECE):
        def piece(m):
            return jnp.concatenate([w[m, k, q * zs : (q + 1) * zs].reshape(PIECE, -1) for k in range(ks)], axis=1)

        nt = (((1,), (1,)), ((), ()))
        value = lax.dot_general(tok[...], piece(0), nt, preferred_element_type=jnp.float32)
        gate = lax.dot_general(tok[...], piece(1), nt, preferred_element_type=jnp.float32)
        glu = (value * jax.nn.sigmoid(gate)).astype(jnp.bfloat16).astype(jnp.float32)
        shifted[0] = glu
        for r in range(1, 8):
            shifted[r] = pltpu.roll(glu, r, 0)
        half = rows // 2
        for l in range(PIECE // LANES):
            lanes = slice(l * LANES, (l + 1) * LANES)
            here = slice(q * PIECE + l * LANES, q * PIECE + (l + 1) * LANES)
            for h in range(2):
                acc = jnp.zeros((half, LANES), jnp.float32)
                for k in range(taps):
                    r, j = k % 8, k // 8
                    begin = HALO - 8 * j + h * half
                    acc = acc + cw_ref[k : k + 1, here] * shifted[r, begin : begin + half, lanes]
                acc = acc.astype(jnp.bfloat16)
                span = slice(h * half, (h + 1) * half)
                conv[span, here] = acc
                acc = acc.astype(jnp.float32)
                if q == 0 and l == 0:
                    sums[span] = acc
                    squares[span] = acc * acc
                else:
                    sums[span] += acc
                    squares[span] += acc * acc

    mean = jnp.sum(sums[...], axis=1, keepdims=True) / channels
    meansq = jnp.sum(squares[...], axis=1, keepdims=True) / channels
    scale = lax.rsqrt(meansq - mean * mean + EPS)
    for q in range(channels // PIECE):
        here = slice(q * PIECE, (q + 1) * PIECE)
        v = (conv[:, here].astype(jnp.float32) - mean) * scale * gain_ref[:, here] + bias_ref[:, here]
        conv[:, here] = (v / (1.0 + jnp.exp(-v))).astype(jnp.bfloat16)
    for c in late:
        c.wait()
    normed = conv[...]
    for k in range(ks):
        right = w[2, k].reshape(channels, -1)
        out = jnp.dot(normed, right, preferred_element_type=jnp.float32)
        out_ref[:, k * right.shape[1] : (k + 1) * right.shape[1]] = out.astype(jnp.bfloat16)


def per_device(tokens, w_value, w_gate, conv_weight, norm_gain, norm_bias, w_out):
    rows = tokens[0]
    length, depth = rows.shape
    taps, channels = conv_weight.shape
    positions = lax.axis_size(("zh", "zl"))
    core, side = lax.axis_index("core"), lax.axis_index("side")
    halo = lax.ppermute(rows[length - HALO :], ("zh", "zl"), [(i, i + 1) for i in range(positions - 1)])

    both = jnp.stack([w_value.T, w_gate.T, w_out])
    half = both.shape[1] // 2
    mine = lax.dynamic_slice_in_dim(both, side * half, half, 1)
    far = spread(mine, "zh")
    near = spread(far, "zl")
    near = near.transpose(2, 1, 0, 3, 4).reshape(3, positions, half, -1)
    vg, o = near[:2], near[2]
    vg_other = swapped(vg, "side")
    oa = spread(o, "x")
    ob = swapped(oa, "side")
    vg0 = spread(jnp.stack([vg, vg_other]), "x")
    oa1, ob1 = swapped(oa, "core"), swapped(ob, "core")
    vg1 = swapped(vg0, "core")

    hbm = pl.BlockSpec(memory_space=pl.ANY)
    vmem = pl.BlockSpec(memory_space=pltpu.VMEM)
    blocks = vg0.shape[0]
    mixed = pl.pallas_call(
        body,
        out_shape=jax.ShapeDtypeStruct((length, depth), jnp.bfloat16),
        in_specs=[pl.BlockSpec(memory_space=pltpu.SMEM), hbm, hbm, vmem, vmem, vmem] + [hbm] * 6,
        out_specs=vmem,
        scratch_shapes=[
            pltpu.VMEM((length + HALO, depth), jnp.bfloat16),
            pltpu.VMEM((3, 2 * blocks, positions, 2, half, w_out.shape[1]), jnp.bfloat16),
            pltpu.VMEM((8, length + HALO, PIECE), jnp.float32),
            pltpu.VMEM((length, channels), jnp.bfloat16),
            pltpu.VMEM((length, LANES), jnp.float32),
            pltpu.VMEM((length, LANES), jnp.float32),
            pltpu.SemaphoreType.DMA((2,)),
            pltpu.SemaphoreType.DMA((8 * blocks,)),
            pltpu.SemaphoreType.DMA((4 * blocks,)),
        ],
        compiler_params=pltpu.CompilerParams(vmem_limit_bytes=48 * 1024 * 1024),
        cost_estimate=pl.CostEstimate(flops=6 * length * depth * channels, bytes_accessed=16 * 1024 * 1024, transcendentals=0),
        name="conv_module",
    )(
        jnp.stack([core, side]).astype(jnp.int32), halo, rows, conv_weight.astype(jnp.float32),
        norm_gain[None], norm_bias[None], vg0, vg1, oa, ob, oa1, ob1,
    )
    return mixed[None]


def solution(mesh):
    groups, positions, columns = (mesh.shape[a] for a in ("grp", "sp", "dp"))
    fine = Mesh(
        mesh.devices.reshape(groups // 2, 2, positions // 4, 4, columns // 2, 2),
        ("pair", "side", "zh", "zl", "x", "core"),
    )
    z, dp = ("zh", "zl"), ("x", "core")
    placed = (
        P(("pair", "side", *dp), z, None),
        P(dp, z),
        P(dp, z),
        P(),
        P(),
        P(),
        P(z, dp),
    )
    return jax.shard_map(
        per_device,
        mesh=fine,
        in_specs=placed,
        out_specs=P(("pair", "side", *dp), z, None),
        check_vma=False,
    )
```

```python
import jax
import jax.numpy as jnp
from jax import lax
from jax.experimental import pallas as pl
from jax.experimental.pallas import tpu as pltpu
from jax.sharding import Mesh, PartitionSpec as P


EPS = 1e-05
HALO = 32
PIECE = 256
LANES = 128


def spread(block, axis):
    members = lax.axis_size(axis)
    return lax.all_to_all(jnp.broadcast_to(block, (members, *block.shape)), axis, 0, 0)


def swapped(array, axis):
    return lax.ppermute(array, axis, [(0, 1), (1, 0)])


def columns(where_ref, x, m, deep):
    core = where_ref[0]
    c = core if m == 0 else 1 - core
    return pl.ds(pl.multiple_of((2 * x + c) * deep, deep), deep)


def convolve(where_ref, halo_ref, tok_ref, cw_ref, vg0_ref, vg1_ref, conv_ref, stats_ref, tok, shifted):
    par = where_ref[1]
    rows, part = conv_ref.shape
    taps = cw_ref.shape[1]
    blocks, deep = vg0_ref.shape[0], vg0_ref.shape[-1]
    order = [(x, m) for x in range(blocks) for m in range(2)]
    for at, (x, m) in enumerate(order):
        here = slice(at * deep, (at + 1) * deep)
        tok[:HALO, here] = halo_ref[:, columns(where_ref, x, m, deep)]
        tok[HALO:, here] = tok_ref[:, columns(where_ref, x, m, deep)]

    half = rows // 2
    for q in range(part // PIECE):
        span = slice(q * PIECE, (q + 1) * PIECE)

        def product(m):
            piece = jnp.concatenate([(vg0_ref, vg1_ref)[c][x, m, span, :] for x, c in order], axis=1)
            return lax.dot_general(tok[...], piece, (((1,), (1,)), ((), ())), preferred_element_type=jnp.float32)

        value, gate = product(0), product(1)
        glu = (value * jax.nn.sigmoid(gate)).astype(jnp.bfloat16).astype(jnp.float32)
        shifted[0] = glu
        for r in range(1, 8):
            shifted[r] = pltpu.roll(glu, r, 0)
        for l in range(PIECE // LANES):
            lanes = slice(l * LANES, (l + 1) * LANES)
            at = q * PIECE + l * LANES
            for h in range(2):
                acc = jnp.zeros((half, LANES), jnp.float32)
                for k in range(taps):
                    r, j = k % 8, k // 8
                    begin = HALO - 8 * j + h * half
                    acc = acc + cw_ref[par, k : k + 1, at : at + LANES] * shifted[r, begin : begin + half, lanes]
                acc = acc.astype(jnp.bfloat16)
                when = slice(h * half, (h + 1) * half)
                conv_ref[when, at : at + LANES] = acc
                acc = acc.astype(jnp.float32)
                if q == 0 and l == 0:
                    stats_ref[0, when] = acc
                    stats_ref[1, when] = acc * acc
                else:
                    stats_ref[0, when] += acc
                    stats_ref[1, when] += acc * acc


def finish(where_ref, conv_a_ref, conv_b_ref, stats_a_ref, stats_b_ref, gain_ref, bias_ref, o0_ref, o1_ref, out_ref, normed):
    side = where_ref[1]
    part = conv_a_ref.shape[1]
    blocks, deep = o0_ref.shape[1], o0_ref.shape[-1]
    mean = jnp.sum(stats_a_ref[0] + stats_b_ref[0], axis=1, keepdims=True) / (2 * part)
    meansq = jnp.sum(stats_a_ref[1] + stats_b_ref[1], axis=1, keepdims=True) / (2 * part)
    scale = lax.rsqrt(meansq - mean * mean + EPS)
    for s, conv_ref in enumerate((conv_a_ref, conv_b_ref)):
        par = side if s == 0 else 1 - side
        for q in range(part // PIECE):
            span = slice(q * PIECE, (q + 1) * PIECE)
            v = (conv_ref[:, span].astype(jnp.float32) - mean) * scale * gain_ref[par, :, span] + bias_ref[par, :, span]
            here = slice(s * part + q * PIECE, s * part + (q + 1) * PIECE)
            normed[:, here] = (v / (1.0 + jnp.exp(-v))).astype(jnp.bfloat16)
    for x in range(blocks):
        for m, o_ref in enumerate((o0_ref, o1_ref)):
            right = jnp.concatenate([o_ref[0, x], o_ref[1, x]], axis=0)
            out = jnp.dot(normed[...], right, preferred_element_type=jnp.float32)
            out_ref[:, columns(where_ref, x, m, deep)] = out.astype(jnp.bfloat16)


SMEM, VMEM = (pl.BlockSpec(memory_space=space) for space in (pltpu.SMEM, pltpu.VMEM))


def kernel(function, out_shape, scratch, flops, mib, *operands):
    single = not isinstance(out_shape, tuple)
    return pl.pallas_call(
        function,
        out_shape=out_shape,
        in_specs=[SMEM] + [VMEM] * (len(operands) - 1),
        out_specs=VMEM if single else (VMEM,) * len(out_shape),
        scratch_shapes=scratch,
        compiler_params=pltpu.CompilerParams(vmem_limit_bytes=mib * 1024 * 1024),
        cost_estimate=pl.CostEstimate(flops=flops, bytes_accessed=8 * 1024 * 1024, transcendentals=0),
    )(*operands)


def by_side(array, positions):
    k = array.shape[0]
    return array.reshape(k, positions, 2, -1).transpose(2, 0, 1, 3).reshape(2, k, -1)


def per_device(tokens, w_value, w_gate, conv_weight, norm_gain, norm_bias, w_out):
    rows = tokens[0]
    length, depth = rows.shape
    channels = conv_weight.shape[1]
    positions = lax.axis_size(("zh", "zl"))
    core, side = lax.axis_index("core"), lax.axis_index("side")
    both = jnp.stack([w_value.T, w_gate.T, w_out])
    half = both.shape[1] // 2
    mine = lax.dynamic_slice_in_dim(both, side * half, half, 1)
    far = lax.all_gather(mine, "zh", axis=0, tiled=True)
    near = lax.all_gather(far, "zl", axis=0, tiled=True)
    near = near.reshape(lax.axis_size("zl"), lax.axis_size("zh"), *mine.shape)
    near = near.transpose(2, 1, 0, 3, 4).reshape(3, positions * half, -1)
    last = rows[length - HALO :]
    near, last, conv_weight, norm_gain, norm_bias = lax.optimization_barrier((near, last, conv_weight, norm_gain, norm_bias))
    vg, o = near[:2], near[2]
    vg_other = swapped(vg, "side")
    halo = lax.ppermute(last, ("zh", "zl"), [(i, i + 1) for i in range(positions - 1)])
    oa = spread(o, "x")
    ob = swapped(oa, "side")
    vga0 = spread(vg, "x")
    vga1 = swapped(vga0, "core")
    vgb0 = spread(vg_other, "x")
    vgb1 = swapped(vgb0, "core")
    o0 = jnp.stack([oa, ob])
    o1 = swapped(o0, "core")
    taps = by_side(conv_weight.astype(jnp.float32), positions)
    gain, bias = by_side(norm_gain[None], positions), by_side(norm_bias[None], positions)
    here, there = (jnp.stack([core, s]).astype(jnp.int32) for s in (side, 1 - side))
    part = channels // 2
    made = (jax.ShapeDtypeStruct((length, part), jnp.bfloat16), jax.ShapeDtypeStruct((2, length, LANES), jnp.float32))
    scratch = [
        pltpu.VMEM((length + HALO, depth), jnp.bfloat16),
        pltpu.VMEM((8, length + HALO, PIECE), jnp.float32),
    ]
    flops = 2 * length * depth * channels
    conv_a, stats_a = kernel(convolve, made, scratch, flops, 20, here, halo, rows, taps, vga0, vga1)
    conv_b, stats_b = kernel(convolve, made, scratch, flops, 20, there, halo, rows, taps, vgb0, vgb1)
    mixed = kernel(
        finish, jax.ShapeDtypeStruct((length, depth), jnp.bfloat16),
        [pltpu.VMEM((length, channels), jnp.bfloat16)], flops, 16,
        here, conv_a, conv_b, stats_a, stats_b, gain, bias, o0, o1,
    )
    return mixed[None]


def solution(mesh):
    groups, positions, columns = (mesh.shape[a] for a in ("grp", "sp", "dp"))
    fine = Mesh(
        mesh.devices.reshape(groups // 2, 2, positions // 2, 2, columns // 2, 2),
        ("pair", "side", "zh", "zl", "x", "core"),
    )
    z, dp = ("zh", "zl"), ("x", "core")
    placed = (
        P(("pair", "side", *dp), z, None),
        P(dp, z),
        P(dp, z),
        P(),
        P(),
        P(),
        P(z, dp),
    )
    return jax.shard_map(
        per_device,
        mesh=fine,
        in_specs=placed,
        out_specs=P(("pair", "side", *dp), z, None),
        check_vma=False,
    )
```

```python
import jax
import jax.numpy as jnp
from jax import lax
from jax.experimental import pallas as pl
from jax.experimental.pallas import tpu as pltpu
from jax.sharding import Mesh, PartitionSpec as P


EPS = 1e-05
HALO = 32
PIECE = 256
LANES = 128


def spread(block, axis):
    members = lax.axis_size(axis)
    return lax.all_to_all(jnp.broadcast_to(block, (members, *block.shape)), axis, 0, 0)


def swapped(array, axis):
    return lax.ppermute(array, axis, [(0, 1), (1, 0)])


def columns(where_ref, x, m, deep):
    core = where_ref[0]
    c = core if m == 0 else 1 - core
    return pl.ds(pl.multiple_of((2 * x + c) * deep, deep), deep)


def chosen(array, par, precision=None):
    wide, width = 2 * LANES, LANES // 8
    source = lax.broadcasted_iota(jnp.int32, (wide, LANES), 0)
    target = lax.broadcasted_iota(jnp.int32, (wide, LANES), 1)
    pick = source == (target // width) * (2 * width) + par * width + target % width
    pick = jnp.where(pick, 1.0, 0.0).astype(array.dtype)
    parts = [array[:, at : at + wide] for at in range(0, array.shape[1], wide)]
    parts = [jnp.dot(p, pick, preferred_element_type=jnp.float32, precision=precision) for p in parts]
    return jnp.concatenate(parts, axis=1)


def convolve(where_ref, halo_ref, tok_ref, cw_ref, v0_ref, v1_ref, g0_ref, g1_ref, conv_ref, stats_ref, tok, shifted, cw):
    par = where_ref[1]
    rows, part = conv_ref.shape
    taps = cw_ref.shape[0]
    blocks, deep = v0_ref.shape[0], v0_ref.shape[-1]
    order = [(x, m) for x in range(blocks) for m in range(2)]
    for at, (x, m) in enumerate(order):
        here = slice(at * deep, (at + 1) * deep)
        tok[:HALO, here] = halo_ref[:, columns(where_ref, x, m, deep)]
        tok[HALO:, here] = tok_ref[:, columns(where_ref, x, m, deep)]
    cw[...] = chosen(cw_ref[...], par)

    half = rows // 2
    for q in range(part // PIECE):
        span = slice(q * PIECE, (q + 1) * PIECE)

        def product(*refs):
            piece = jnp.concatenate([refs[m][x, span, :] for x, m in order], axis=1)
            return lax.dot_general(tok[...], piece, (((1,), (1,)), ((), ())), preferred_element_type=jnp.float32)

        value, gate = product(v0_ref, v1_ref), product(g0_ref, g1_ref)
        glu = (value * jax.nn.sigmoid(gate)).astype(jnp.bfloat16).astype(jnp.float32)
        shifted[0] = glu
        for r in range(1, 8):
            shifted[r] = pltpu.roll(glu, r, 0)
        for l in range(PIECE // LANES):
            lanes = slice(l * LANES, (l + 1) * LANES)
            at = q * PIECE + l * LANES
            for h in range(2):
                acc = jnp.zeros((half, LANES), jnp.float32)
                for k in range(taps):
                    r, j = k % 8, k // 8
                    begin = HALO - 8 * j + h * half
                    acc = acc + cw[k : k + 1, at : at + LANES] * shifted[r, begin : begin + half, lanes]
                acc = acc.astype(jnp.bfloat16)
                when = slice(h * half, (h + 1) * half)
                conv_ref[when, at : at + LANES] = acc
                acc = acc.astype(jnp.float32)
                if q == 0 and l == 0:
                    stats_ref[0, when] = acc
                    stats_ref[1, when] = acc * acc
                else:
                    stats_ref[0, when] += acc
                    stats_ref[1, when] += acc * acc


def finish(
    where_ref, conv_a_ref, conv_b_ref, stats_a_ref, stats_b_ref, gain_ref, bias_ref,
    oa0_ref, ob0_ref, oa1_ref, ob1_ref, out_ref, normed,
):
    side = where_ref[1]
    part = conv_a_ref.shape[1]
    blocks, deep = oa0_ref.shape[0], oa0_ref.shape[-1]
    mean = jnp.sum(stats_a_ref[0] + stats_b_ref[0], axis=1, keepdims=True) / (2 * part)
    meansq = jnp.sum(stats_a_ref[1] + stats_b_ref[1], axis=1, keepdims=True) / (2 * part)
    scale = lax.rsqrt(meansq - mean * mean + EPS)
    for s, conv_ref in enumerate((conv_a_ref, conv_b_ref)):
        par = side if s == 0 else 1 - side
        gain = chosen(jnp.broadcast_to(gain_ref[...], (8, 2 * part)), par, lax.Precision.HIGHEST)[:1]
        bias = chosen(jnp.broadcast_to(bias_ref[...], (8, 2 * part)), par, lax.Precision.HIGHEST)[:1]
        for q in range(part // PIECE):
            span = slice(q * PIECE, (q + 1) * PIECE)
            v = (conv_ref[:, span].astype(jnp.float32) - mean) * scale * gain[:, span] + bias[:, span]
            here = slice(s * part + q * PIECE, s * part + (q + 1) * PIECE)
            normed[:, here] = (v / (1.0 + jnp.exp(-v))).astype(jnp.bfloat16)
    for x in range(blocks):
        for m, (own, other) in enumerate(((oa0_ref, ob0_ref), (oa1_ref, ob1_ref))):
            right = jnp.concatenate([own[x], other[x]], axis=0)
            out = jnp.dot(normed[...], right, preferred_element_type=jnp.float32)
            out_ref[:, columns(where_ref, x, m, deep)] = out.astype(jnp.bfloat16)


SMEM, VMEM = (pl.BlockSpec(memory_space=space) for space in (pltpu.SMEM, pltpu.VMEM))


def kernel(function, out_shape, scratch, flops, mib, *operands):
    single = not isinstance(out_shape, tuple)
    return pl.pallas_call(
        function,
        out_shape=out_shape,
        in_specs=[SMEM] + [VMEM] * (len(operands) - 1),
        out_specs=VMEM if single else (VMEM,) * len(out_shape),
        scratch_shapes=scratch,
        compiler_params=pltpu.CompilerParams(vmem_limit_bytes=mib * 1024 * 1024),
        cost_estimate=pl.CostEstimate(flops=flops, bytes_accessed=8 * 1024 * 1024, transcendentals=0),
    )(*operands)


def per_device(tokens, w_value, w_gate, conv_weight, norm_gain, norm_bias, w_out):
    rows = tokens[0]
    length, depth = rows.shape
    channels = conv_weight.shape[1]
    positions = lax.axis_size(("zh", "zl"))
    core, side = lax.axis_index("core"), lax.axis_index("side")
    both = jnp.stack([w_value.T, w_gate.T, w_out])
    half = both.shape[1] // 2
    mine = lax.dynamic_slice_in_dim(both, side * half, half, 1)
    far = lax.all_gather(mine, "zh", axis=0, tiled=True)
    near = lax.all_gather(far, "zl", axis=0, tiled=True)
    near = near.reshape(lax.axis_size("zl"), lax.axis_size("zh"), *mine.shape)
    near = near.transpose(2, 1, 0, 3, 4).reshape(3, positions * half, -1)
    last = rows[length - HALO :]
    near, last, conv_weight, norm_gain, norm_bias = lax.optimization_barrier((near, last, conv_weight, norm_gain, norm_bias))
    v, g, o = near

    ga0 = spread(g, "x")
    v_other = swapped(v, "side")
    halo = lax.ppermute(last, ("zh", "zl"), [(i, i + 1) for i in range(positions - 1)])
    oa0 = spread(o, "x")
    gb0 = swapped(ga0, "side")
    ga1 = swapped(ga0, "core")
    va0 = spread(v, "x")
    ob0 = swapped(oa0, "side")
    oa1 = swapped(oa0, "core")
    vb0 = spread(v_other, "x")
    va1 = swapped(va0, "core")
    gb1 = swapped(gb0, "core")
    vb1 = swapped(vb0, "core")
    ob1 = swapped(ob0, "core")
    here, there = (jnp.stack([core, s]).astype(jnp.int32) for s in (side, 1 - side))
    part = channels // 2
    made = (jax.ShapeDtypeStruct((length, part), jnp.bfloat16), jax.ShapeDtypeStruct((2, length, LANES), jnp.float32))
    scratch = [
        pltpu.VMEM((length + HALO, depth), jnp.bfloat16),
        pltpu.VMEM((8, length + HALO, PIECE), jnp.float32),
        pltpu.VMEM((conv_weight.shape[0], part), jnp.float32),
    ]
    flops = 2 * length * depth * channels
    conv_a, stats_a = kernel(convolve, made, scratch, flops, 20, here, halo, rows, conv_weight, va0, va1, ga0, ga1)
    conv_b, stats_b = kernel(convolve, made, scratch, flops, 20, there, halo, rows, conv_weight, vb0, vb1, gb0, gb1)
    mixed = kernel(
        finish, jax.ShapeDtypeStruct((length, depth), jnp.bfloat16),
        [pltpu.VMEM((length, channels), jnp.bfloat16)], flops, 16,
        here, conv_a, conv_b, stats_a, stats_b, norm_gain[None], norm_bias[None], oa0, ob0, oa1, ob1,
    )
    return mixed[None]


def solution(mesh):
    groups, positions, columns = (mesh.shape[a] for a in ("grp", "sp", "dp"))
    fine = Mesh(
        mesh.devices.reshape(groups // 2, 2, positions // 2, 2, columns // 2, 2),
        ("pair", "side", "zh", "zl", "x", "core"),
    )
    z, dp = ("zh", "zl"), ("x", "core")
    placed = (
        P(("pair", "side", *dp), z, None),
        P(dp, z),
        P(dp, z),
        P(),
        P(),
        P(),
        P(z, dp),
    )
    return jax.shard_map(
        per_device,
        mesh=fine,
        in_specs=placed,
        out_specs=P(("pair", "side", *dp), z, None),
        check_vma=False,
    )
```

```python
import jax
import jax.numpy as jnp
from jax import lax
from jax.experimental import pallas as pl
from jax.experimental.pallas import tpu as pltpu
from jax.sharding import Mesh, PartitionSpec as P


EPS = 1e-05
HALO = 32
PIECE = 256
LANES = 128


def copies(block, axis):
    return jnp.broadcast_to(block, (lax.axis_size(axis), *block.shape))


def exchanged(blocks, axis):
    return lax.all_to_all(blocks, axis, 0, 0)


def swapped(array, axis):
    return lax.ppermute(array, axis, [(0, 1), (1, 0)])


def columns(where_ref, x, m, deep):
    core = where_ref[0]
    c = core if m == 0 else 1 - core
    return pl.ds(pl.multiple_of((2 * x + c) * deep, deep), deep)


def chosen(array, par, precision=None):
    wide, width = 2 * LANES, LANES // 8
    source = lax.broadcasted_iota(jnp.int32, (wide, LANES), 0)
    target = lax.broadcasted_iota(jnp.int32, (wide, LANES), 1)
    pick = source == (target // width) * (2 * width) + par * width + target % width
    pick = jnp.where(pick, 1.0, 0.0).astype(array.dtype)
    parts = [array[:, at : at + wide] for at in range(0, array.shape[1], wide)]
    parts = [jnp.dot(p, pick, preferred_element_type=jnp.float32, precision=precision) for p in parts]
    return jnp.concatenate(parts, axis=1)


def prepare(where_ref, halo_ref, tok_ref, cw_ref, tok, cw):
    deep = tok_ref.shape[1] // 8
    for at in range(8):
        here = slice(at * deep, (at + 1) * deep)
        tok[:HALO, here] = halo_ref[:, columns(where_ref, at // 2, at % 2, deep)]
        tok[HALO:, here] = tok_ref[:, columns(where_ref, at // 2, at % 2, deep)]
    for s in range(2):
        par = where_ref[1] if s == 0 else 1 - where_ref[1]
        cw[s] = chosen(cw_ref[...], par)


def convolve(s, tok, cw, value_of, g0_ref, g1_ref, conv_ref, stats_ref, shifted):
    rows, part = conv_ref.shape
    taps = cw.shape[1]
    blocks = g0_ref.shape[0]
    order = [(x, m) for x in range(blocks) for m in range(2)]

    half = rows // 2
    for q in range(part // PIECE):
        span = slice(q * PIECE, (q + 1) * PIECE)

        def product(of):
            piece = jnp.concatenate([of(m, x, span) for x, m in order], axis=1)
            return lax.dot_general(tok[...], piece, (((1,), (1,)), ((), ())), preferred_element_type=jnp.float32)

        value, gate = product(value_of), product(lambda m, x, span: (g0_ref, g1_ref)[m][x, span, :])
        glu = (value * jax.nn.sigmoid(gate)).astype(jnp.bfloat16).astype(jnp.float32)
        shifted[0] = glu
        for r in range(1, 8):
            shifted[r] = pltpu.roll(glu, r, 0)
        for l in range(PIECE // LANES):
            lanes = slice(l * LANES, (l + 1) * LANES)
            at = q * PIECE + l * LANES
            for h in range(2):
                acc = jnp.zeros((half, LANES), jnp.float32)
                for k in range(taps):
                    r, j = k % 8, k // 8
                    begin = HALO - 8 * j + h * half
                    acc = acc + cw[s, k : k + 1, at : at + LANES] * shifted[r, begin : begin + half, lanes]
                acc = acc.astype(jnp.bfloat16)
                when = slice(h * half, (h + 1) * half)
                conv_ref[when, at : at + LANES] = acc
                acc = acc.astype(jnp.float32)
                if q == 0 and l == 0:
                    stats_ref[0, when] = acc
                    stats_ref[1, when] = acc * acc
                else:
                    stats_ref[0, when] += acc
                    stats_ref[1, when] += acc * acc


def first_half(where_ref, halo_ref, tok_ref, cw_ref, ov0_ref, ov1_ref, g0_ref, g1_ref, conv_ref, stats_ref, tok, cw, shifted):
    prepare(where_ref, halo_ref, tok_ref, cw_ref, tok, cw)
    convolve(0, tok, cw, lambda m, x, span: (ov0_ref, ov1_ref)[m][x, 1, span, :], g0_ref, g1_ref, conv_ref, stats_ref, shifted)


def second_half(where_ref, tok, cw, v0_ref, v1_ref, g0_ref, g1_ref, conv_ref, stats_ref, shifted):
    convolve(1, tok, cw, lambda m, x, span: (v0_ref, v1_ref)[m][x, span, :], g0_ref, g1_ref, conv_ref, stats_ref, shifted)


def finish(
    where_ref, conv_a_ref, conv_b_ref, stats_a_ref, stats_b_ref, gain_ref, bias_ref,
    ov0_ref, ob0_ref, ov1_ref, ob1_ref, out_ref, normed,
):
    side = where_ref[1]
    part = conv_a_ref.shape[1]
    blocks, deep = ob0_ref.shape[0], ob0_ref.shape[-1]
    mean = jnp.sum(stats_a_ref[0] + stats_b_ref[0], axis=1, keepdims=True) / (2 * part)
    meansq = jnp.sum(stats_a_ref[1] + stats_b_ref[1], axis=1, keepdims=True) / (2 * part)
    scale = lax.rsqrt(meansq - mean * mean + EPS)
    for s, conv_ref in enumerate((conv_a_ref, conv_b_ref)):
        par = side if s == 0 else 1 - side
        gain = chosen(jnp.broadcast_to(gain_ref[...], (8, 2 * part)), par, lax.Precision.HIGHEST)[:1]
        bias = chosen(jnp.broadcast_to(bias_ref[...], (8, 2 * part)), par, lax.Precision.HIGHEST)[:1]
        for q in range(part // PIECE):
            span = slice(q * PIECE, (q + 1) * PIECE)
            v = (conv_ref[:, span].astype(jnp.float32) - mean) * scale * gain[:, span] + bias[:, span]
            here = slice(s * part + q * PIECE, s * part + (q + 1) * PIECE)
            normed[:, here] = (v / (1.0 + jnp.exp(-v))).astype(jnp.bfloat16)
    for x in range(blocks):
        for m, (own, other) in enumerate(((ov0_ref, ob0_ref), (ov1_ref, ob1_ref))):
            right = jnp.concatenate([own[x, 0], other[x]], axis=0)
            out = jnp.dot(normed[...], right, preferred_element_type=jnp.float32)
            out_ref[:, columns(where_ref, x, m, deep)] = out.astype(jnp.bfloat16)


SMEM, VMEM = (pl.BlockSpec(memory_space=space) for space in (pltpu.SMEM, pltpu.VMEM))


def kernel(function, out_shape, scratch, flops, mib, *operands):
    single = not isinstance(out_shape, tuple)
    return pl.pallas_call(
        function,
        out_shape=out_shape,
        in_specs=[SMEM] + [VMEM] * (len(operands) - 1),
        out_specs=VMEM if single else (VMEM,) * len(out_shape),
        scratch_shapes=scratch,
        compiler_params=pltpu.CompilerParams(vmem_limit_bytes=mib * 1024 * 1024),
        cost_estimate=pl.CostEstimate(flops=flops, bytes_accessed=8 * 1024 * 1024, transcendentals=0),
    )(*operands)


def per_device(tokens, w_value, w_gate, conv_weight, norm_gain, norm_bias, w_out):
    rows = tokens[0]
    length, depth = rows.shape
    channels = conv_weight.shape[1]
    positions = lax.axis_size(("zh", "zl"))
    core, side = lax.axis_index("core"), lax.axis_index("side")
    both = jnp.stack([w_value.T, w_gate.T, w_out])
    half = both.shape[1] // 2
    mine = lax.dynamic_slice_in_dim(both, side * half, half, 1)
    far = lax.all_gather(mine, "zh", axis=0, tiled=True)
    near = lax.all_gather(far, "zl", axis=0, tiled=True)
    near = near.reshape(lax.axis_size("zl"), lax.axis_size("zh"), *mine.shape)
    near = near.transpose(2, 1, 0, 3, 4).reshape(3, positions * half, -1)
    last = rows[length - HALO :]
    near, last, conv_weight, norm_gain, norm_bias = lax.optimization_barrier((near, last, conv_weight, norm_gain, norm_bias))
    v, g, o = near

    ga0 = exchanged(copies(g, "x"), "x")
    v_other = swapped(v, "side")
    halo = lax.ppermute(last, ("zh", "zl"), [(i, i + 1) for i in range(positions - 1)])
    ov0 = exchanged(copies(jnp.stack([o, v]), "x"), "x")
    gb0 = swapped(ga0, "side")
    ga1 = swapped(ga0, "core")
    ob0 = swapped(ov0[:, 0], "side")
    vb0 = exchanged(copies(v_other, "x"), "x")
    ov1 = swapped(ov0, "core")
    gb1 = swapped(gb0, "core")
    vb1 = swapped(vb0, "core")
    ob1 = swapped(ob0, "core")
    where = jnp.stack([core, side]).astype(jnp.int32)
    part = channels // 2
    shape = jax.ShapeDtypeStruct
    made = (shape((length, part), jnp.bfloat16), shape((2, length, LANES), jnp.float32))
    ready = (shape((length + HALO, depth), jnp.bfloat16), shape((2, conv_weight.shape[0], part), jnp.float32))
    scratch = [pltpu.VMEM((8, length + HALO, PIECE), jnp.float32)]
    flops = 2 * length * depth * channels
    conv_a, stats_a, tok, cw = kernel(
        first_half, made + ready, scratch, flops, 20,
        where, halo, rows, conv_weight, ov0, ov1, ga0, ga1,
    )
    conv_b, stats_b = kernel(second_half, made, scratch, flops, 20, where, tok, cw, vb0, vb1, gb0, gb1)
    mixed = kernel(
        finish, jax.ShapeDtypeStruct((length, depth), jnp.bfloat16),
        [pltpu.VMEM((length, channels), jnp.bfloat16)], flops, 16,
        where, conv_a, conv_b, stats_a, stats_b, norm_gain[None], norm_bias[None], ov0, ob0, ov1, ob1,
    )
    return mixed[None]


def solution(mesh):
    groups, positions, columns = (mesh.shape[a] for a in ("grp", "sp", "dp"))
    fine = Mesh(
        mesh.devices.reshape(groups // 2, 2, positions // 2, 2, columns // 2, 2),
        ("pair", "side", "zh", "zl", "x", "core"),
    )
    z, dp = ("zh", "zl"), ("x", "core")
    placed = (
        P(("pair", "side", *dp), z, None),
        P(dp, z),
        P(dp, z),
        P(),
        P(),
        P(),
        P(z, dp),
    )
    return jax.shard_map(
        per_device,
        mesh=fine,
        in_specs=placed,
        out_specs=P(("pair", "side", *dp), z, None),
        check_vma=False,
    )
```

```python
import jax
import jax.numpy as jnp
from jax import lax
from jax.experimental import pallas as pl
from jax.experimental.pallas import tpu as pltpu
from jax.sharding import Mesh, PartitionSpec as P


EPS = 1e-05
HALO = 32
LANES = 128
QUARTERS = ((0, 0), (1, 0), (0, 1), (1, 1))


def copies(block, axis):
    return jnp.broadcast_to(block, (lax.axis_size(axis), *block.shape))


def exchanged(blocks, axis):
    return lax.all_to_all(blocks, axis, 0, 0)


def swapped(array, axis):
    return lax.ppermute(array, axis, [(0, 1), (1, 0)])


def columns(where_ref, x, m, deep):
    core = where_ref[0]
    c = core if m == 0 else 1 - core
    return pl.ds(pl.multiple_of((2 * x + c) * deep, deep), deep)


def chosen(array, where_ref, quarter, precision=None):
    side = where_ref[1] if quarter[0] == 0 else 1 - where_ref[1]
    parity = where_ref[2] if quarter[1] == 0 else 1 - where_ref[2]
    width = LANES // 8
    wide = 4 * LANES
    source = lax.broadcasted_iota(jnp.int32, (wide, LANES), 0)
    target = lax.broadcasted_iota(jnp.int32, (wide, LANES), 1)
    pick = source == (target // width) * (4 * width) + parity * (2 * width) + side * width + target % width
    pick = jnp.where(pick, 1.0, 0.0).astype(array.dtype)
    parts = [array[:, at : at + wide] for at in range(0, array.shape[1], wide)]
    parts = [jnp.dot(p, pick, preferred_element_type=jnp.float32, precision=precision) for p in parts]
    return jnp.concatenate(parts, axis=1)


def convolve(fresh, tok, cw, value, gate, conv_ref, stats_ref, shifted):
    rows, part = conv_ref.shape[0], value.shape[0]
    taps = cw.shape[1]
    nt = (((1,), (1,)), ((), ()))
    value = lax.dot_general(tok[...], value, nt, preferred_element_type=jnp.float32)
    gate = lax.dot_general(tok[...], gate, nt, preferred_element_type=jnp.float32)
    glu = (value * jax.nn.sigmoid(gate)).astype(jnp.bfloat16).astype(jnp.float32)
    shifted[0] = glu
    for r in range(1, 8):
        shifted[r] = pltpu.roll(glu, r, 0)
    half = rows // 2
    for at in range(0, part, LANES):
        here = slice(at, at + LANES)
        for h in range(2):
            acc = jnp.zeros((half, LANES), jnp.float32)
            for k in range(taps):
                r, j = k % 8, k // 8
                begin = HALO - 8 * j + h * half
                acc = acc + cw[0, k : k + 1, here] * shifted[r, begin : begin + half, here]
            acc = acc.astype(jnp.bfloat16)
            when = slice(h * half, (h + 1) * half)
            conv_ref[when, here] = acc
            acc = acc.astype(jnp.float32)
            if fresh and at == 0:
                stats_ref[0, when] = acc
                stats_ref[1, when] = acc * acc
            else:
                stats_ref[0, when] += acc
                stats_ref[1, when] += acc * acc


def joined(w, blocks, *index):
    return jnp.concatenate([w[(m, x, *index)] for x in range(blocks) for m in range(2)], axis=1)


def first(where_ref, halo_ref, tok_ref, cw_ref, w0_ref, w1_ref, conv_ref, stats_ref, tok_out, cw_out, tok, cw, w, shifted, taps, sems):
    blocks = w.shape[1]
    rows, deep = tok_ref.shape[0], tok.shape[1] // (2 * blocks)
    loads = [pltpu.make_async_copy(cw_ref, taps, sems.at[0])]
    for at in range(2 * blocks):
        here, there = pl.ds(at * deep, deep), columns(where_ref, at // 2, at % 2, deep)
        loads.append(pltpu.make_async_copy(halo_ref.at[:, there], tok.at[pl.ds(0, HALO), here], sems.at[5 + 2 * at]))
        loads.append(pltpu.make_async_copy(tok_ref.at[:, there], tok.at[pl.ds(HALO, rows), here], sems.at[6 + 2 * at]))
    for m, r in enumerate((w0_ref, w1_ref)):
        loads.append(pltpu.make_async_copy(r.at[:, pl.ds(0, 2)], w.at[m], sems.at[1 + m]))
    for load in loads:
        load.start()
    loads[0].wait()
    for i, quarter in enumerate(QUARTERS):
        cw[i] = chosen(taps[...], where_ref, quarter)
    for load in loads[1:]:
        load.wait()
    stores = [pltpu.make_async_copy(tok, tok_out, sems.at[3]), pltpu.make_async_copy(cw, cw_out, sems.at[4])]
    for store in stores:
        store.start()
    convolve(True, tok, cw.at[pl.ds(0, 1)], joined(w, blocks, 0), joined(w, blocks, 1), conv_ref, stats_ref, shifted)
    for store in stores:
        store.wait()


def remaining(where_ref, tok_ref, cw_ref, w0_ref, w1_ref, first_ref, stats_ref, gain_ref, bias_ref, *refs):
    o_refs, (out_ref, tok, cw, w, shifted, conv, whole, stats, more, affine, o, sems) = refs[:-12], refs[-12:]
    count, blocks, part, deep = w.shape[0], w.shape[2], w.shape[4], w.shape[5]
    channels = whole.shape[1]
    serial = iter(range(64))

    def load(source, target):
        copy = pltpu.make_async_copy(source, target, sems.at[next(serial)])
        copy.start()
        return copy

    early = [load(tok_ref, tok), load(cw_ref, cw)]
    pieces = [[load(r.at[:, i], w.at[i, m]) for m, r in enumerate((w0_ref, w1_ref))] for i in range(count)]
    middle = [load(first_ref, conv.at[0]), load(stats_ref, stats)]
    middle += [load(gain_ref, affine.at[pl.ds(0, 1)]), load(bias_ref, affine.at[pl.ds(8, 1)])]
    late = []
    for i, r in enumerate(o_refs):
        m, q = i // len(QUARTERS), i % len(QUARTERS)
        late.append(load(r.at[:, 2] if q == 0 else r, o.at[m, q]))
    for copy in early:
        copy.wait()
    for i in range(count):
        for copy in pieces[i]:
            copy.wait()
        piece = w.at[i]
        value, gate = joined(piece, blocks, 0), joined(piece, blocks, 1)
        convolve(i == 0, tok, cw.at[pl.ds(1 + i, 1)], value, gate, conv.at[1 + i], more, shifted)
    for copy in middle:
        copy.wait()
    mean = jnp.sum(stats[0] + more[0], axis=1, keepdims=True) / channels
    meansq = jnp.sum(stats[1] + more[1], axis=1, keepdims=True) / channels
    scale = lax.rsqrt(meansq - mean * mean + EPS)
    for q, quarter in enumerate(QUARTERS):
        gain, bias = (
            chosen(jnp.broadcast_to(affine[at : at + 1], (8, channels)), where_ref, quarter, lax.Precision.HIGHEST)[:1]
            for at in (0, 8)
        )
        v = (conv[q].astype(jnp.float32) - mean) * scale * gain + bias
        whole[:, q * part : (q + 1) * part] = (v / (1.0 + jnp.exp(-v))).astype(jnp.bfloat16)
    for copy in late:
        copy.wait()
    for x in range(blocks):
        for m in range(2):
            right = jnp.concatenate([o[m, q, x] for q in range(len(QUARTERS))], axis=0)
            out = jnp.dot(whole[...], right, preferred_element_type=jnp.float32)
            out_ref[:, columns(where_ref, x, m, deep)] = out.astype(jnp.bfloat16)


SMEM, VMEM, HBM, ANY = (pl.BlockSpec(memory_space=space) for space in (pltpu.SMEM, pltpu.VMEM, pltpu.HBM, pl.ANY))


def kernel(function, specs, outs, scratch, flops, mib, *operands):
    return pl.pallas_call(
        function,
        out_shape=[o[0] for o in outs],
        in_specs=specs,
        out_specs=[o[1] for o in outs],
        scratch_shapes=scratch,
        compiler_params=pltpu.CompilerParams(vmem_limit_bytes=mib * 1024 * 1024),
        cost_estimate=pl.CostEstimate(flops=flops, bytes_accessed=8 * 1024 * 1024, transcendentals=0),
    )(*operands)


def per_device(tokens, w_value, w_gate, conv_weight, norm_gain, norm_bias, w_out):
    rows = tokens[0]
    length, depth = rows.shape
    taps, channels = conv_weight.shape
    positions = lax.axis_size(("zh", "zl"))
    core, side, parity = (lax.axis_index(a) for a in ("core", "side", "zl"))
    where = jnp.stack([core, side, parity]).astype(jnp.int32)

    both = jnp.stack([w_value.T, w_gate.T, w_out])
    half = both.shape[1] // 2
    mine = lax.dynamic_slice_in_dim(both, side * half, half, 1)
    far = lax.all_gather(mine, "zh", axis=0, tiled=True)
    own = far.reshape(lax.axis_size("zh"), *mine.shape).transpose(1, 0, 2, 3)
    own = own.reshape(3, -1, mine.shape[-1])
    last = rows[length - HALO :]
    own, last, conv_weight, norm_gain, norm_bias = lax.optimization_barrier((own, last, conv_weight, norm_gain, norm_bias))

    vg = own[:2]
    vg_side = swapped(vg, "side")
    own0 = exchanged(copies(own, "x"), "x")
    vg_zl = swapped(jnp.stack([vg, vg_side]), "zl")
    halo = lax.ppermute(last, ("zh", "zl"), [(i, i + 1) for i in range(positions - 1)])
    rest = jnp.concatenate([vg_side[None], vg_zl], axis=0)
    rest0 = exchanged(copies(rest, "x"), "x")
    o00 = own0[:, 2]
    o10 = swapped(o00, "side")
    o01 = swapped(o00, "zl")
    own1 = swapped(own0, "core")
    o11 = swapped(o01, "side")
    o10c = swapped(o10, "core")
    o01c = swapped(o01, "core")
    o11c = swapped(o11, "core")
    rest1 = swapped(rest0, "core")

    shape, vmem, dma = jax.ShapeDtypeStruct, pltpu.VMEM, pltpu.SemaphoreType.DMA
    part, blocks, deep = channels // 4, own0.shape[0], own0.shape[-1]
    tok = ((length + HALO, depth), jnp.bfloat16)
    cw = ((4, taps, part), jnp.float32)
    stats = (shape((2, length, LANES), jnp.float32), VMEM)
    shifted = vmem((8, length + HALO, part), jnp.float32)
    flops = 2 * length * depth * channels // 2
    conv_a, stats_a, tok_ready, cw_ready = kernel(
        first, [SMEM, HBM, HBM, HBM, ANY, ANY],
        [(shape((length, part), jnp.bfloat16), VMEM), stats, (shape(*tok), HBM), (shape(*cw), HBM)],
        [vmem(*tok), vmem(*cw), vmem((2, blocks, 2, part, deep), jnp.bfloat16), shifted,
         vmem((taps, channels), jnp.bfloat16), dma((5 + 4 * blocks,))],
        flops, 56, where, halo, rows, conv_weight, own0, own1,
    )
    (mixed,) = kernel(
        remaining, [SMEM, HBM, HBM, ANY, ANY, HBM, HBM, HBM, HBM] + [ANY] * 8,
        [(shape((length, depth), jnp.bfloat16), VMEM)],
        [vmem(*tok), vmem(*cw), vmem((3, 2, blocks, 2, part, deep), jnp.bfloat16), shifted,
         vmem((4, length, part), jnp.bfloat16), vmem((length, channels), jnp.bfloat16),
         vmem((2, length, LANES), jnp.float32), vmem((2, length, LANES), jnp.float32),
         vmem((16, channels), jnp.float32), vmem((2, 4, blocks, part, deep), jnp.bfloat16), dma((20,))],
        3 * flops, 56, where, tok_ready, cw_ready, rest0, rest1,
        conv_a, stats_a, norm_gain[None], norm_bias[None],
        own0, o10, o01, o11, own1, o10c, o01c, o11c,
    )
    return mixed[None]


def solution(mesh):
    groups, positions, columns = (mesh.shape[a] for a in ("grp", "sp", "dp"))
    fine = Mesh(
        mesh.devices.reshape(groups // 2, 2, positions // 2, 2, columns // 2, 2),
        ("pair", "side", "zh", "zl", "x", "core"),
    )
    z, dp = ("zh", "zl"), ("x", "core")
    placed = (
        P(("pair", "side", *dp), z, None),
        P(dp, z),
        P(dp, z),
        P(),
        P(),
        P(),
        P(z, dp),
    )
    return jax.shard_map(
        per_device,
        mesh=fine,
        in_specs=placed,
        out_specs=P(("pair", "side", *dp), z, None),
        check_vma=False,
    )
```

```python
import jax
import jax.numpy as jnp
from jax import lax
from jax.experimental import pallas as pl
from jax.experimental.pallas import tpu as pltpu
from jax.sharding import Mesh, PartitionSpec as P


EPS = 1e-05
HALO = 32
LANES = 128
QUARTERS = ((0, 0), (1, 0), (0, 1), (1, 1))


def copies(block, axis):
    return jnp.broadcast_to(block, (lax.axis_size(axis), *block.shape))


def exchanged(blocks, axis):
    return lax.all_to_all(blocks, axis, 0, 0)


def swapped(array, axis):
    return lax.ppermute(array, axis, [(0, 1), (1, 0)])


def columns(where_ref, x, m, deep):
    core = where_ref[0]
    c = core if m == 0 else 1 - core
    return pl.ds(pl.multiple_of((2 * x + c) * deep, deep), deep)


def chosen(array, where_ref, quarter, precision=None):
    side = where_ref[1] if quarter[0] == 0 else 1 - where_ref[1]
    parity = where_ref[2] if quarter[1] == 0 else 1 - where_ref[2]
    width = LANES // 8
    wide = 4 * LANES
    source = lax.broadcasted_iota(jnp.int32, (wide, LANES), 0)
    target = lax.broadcasted_iota(jnp.int32, (wide, LANES), 1)
    pick = source == (target // width) * (4 * width) + parity * (2 * width) + side * width + target % width
    pick = jnp.where(pick, 1.0, 0.0).astype(array.dtype)
    parts = [array[:, at : at + wide] for at in range(0, array.shape[1], wide)]
    parts = [jnp.dot(p, pick, preferred_element_type=jnp.float32, precision=precision) for p in parts]
    return jnp.concatenate(parts, axis=1)


def convolve(fresh, tok, cw, value, gate, conv_ref, stats_ref, shifted):
    rows, part = conv_ref.shape[0], value.shape[0]
    taps = cw.shape[1]
    nt = (((1,), (1,)), ((), ()))
    value = lax.dot_general(tok[...], value, nt, preferred_element_type=jnp.float32)
    gate = lax.dot_general(tok[...], gate, nt, preferred_element_type=jnp.float32)
    glu = (value * jax.nn.sigmoid(gate)).astype(jnp.bfloat16).astype(jnp.float32)
    shifted[0] = glu
    for r in range(1, 8):
        shifted[r] = pltpu.roll(glu, r, 0)
    half = rows // 2
    for at in range(0, part, LANES):
        here = slice(at, at + LANES)
        for h in range(2):
            acc = jnp.zeros((half, LANES), jnp.float32)
            for k in range(taps):
                r, j = k % 8, k // 8
                begin = HALO - 8 * j + h * half
                acc = acc + cw[0, k : k + 1, here] * shifted[r, begin : begin + half, here]
            acc = acc.astype(jnp.bfloat16)
            when = slice(h * half, (h + 1) * half)
            conv_ref[when, here] = acc
            acc = acc.astype(jnp.float32)
            if fresh and at == 0:
                stats_ref[0, when] = acc
                stats_ref[1, when] = acc * acc
            else:
                stats_ref[0, when] += acc
                stats_ref[1, when] += acc * acc


def joined(w, blocks, *index):
    return jnp.concatenate([w[(m, x, *index)] for x in range(blocks) for m in range(2)], axis=1)


def first(
    where_ref, halo_ref, tok_ref, cw_ref, gain_ref, bias_ref, w0_ref, w1_ref, conv_ref, stats_ref, tok_out, cw_out, affine_out,
    tok, cw, w, shifted, taps, raw, affine, sems,
):
    blocks = w.shape[1]
    rows, deep = tok_ref.shape[0], tok.shape[1] // (2 * blocks)
    loads = [pltpu.make_async_copy(cw_ref, taps, sems.at[0])]
    for at in range(2 * blocks):
        here, there = pl.ds(at * deep, deep), columns(where_ref, at // 2, at % 2, deep)
        loads.append(pltpu.make_async_copy(halo_ref.at[:, there], tok.at[pl.ds(0, HALO), here], sems.at[8 + 2 * at]))
        loads.append(pltpu.make_async_copy(tok_ref.at[:, there], tok.at[pl.ds(HALO, rows), here], sems.at[9 + 2 * at]))
    for m, r in enumerate((w0_ref, w1_ref)):
        loads.append(pltpu.make_async_copy(r.at[:, pl.ds(0, 2)], w.at[m], sems.at[1 + m]))
    loads.append(pltpu.make_async_copy(gain_ref, raw.at[pl.ds(0, 1)], sems.at[5]))
    loads.append(pltpu.make_async_copy(bias_ref, raw.at[pl.ds(8, 1)], sems.at[6]))
    for load in loads:
        load.start()
    loads[0].wait()
    loads[-2].wait()
    loads[-1].wait()
    pair = jnp.concatenate([raw[0:1], raw[8:9], jnp.zeros((6, raw.shape[1]), jnp.float32)], axis=0)
    part = cw.shape[2]
    for i, quarter in enumerate(QUARTERS):
        cw[i] = chosen(taps[...], where_ref, quarter)
        affine[:, i * part : (i + 1) * part] = chosen(pair, where_ref, quarter, lax.Precision.HIGHEST)
    for load in loads[1:-2]:
        load.wait()
    stores = [
        pltpu.make_async_copy(tok, tok_out, sems.at[3]),
        pltpu.make_async_copy(cw, cw_out, sems.at[4]),
        pltpu.make_async_copy(affine, affine_out, sems.at[7]),
    ]
    for store in stores:
        store.start()
    convolve(True, tok, cw.at[pl.ds(0, 1)], joined(w, blocks, 0), joined(w, blocks, 1), conv_ref, stats_ref, shifted)
    for store in stores:
        store.wait()


def remaining(where_ref, tok_ref, cw_ref, affine_ref, w0_ref, w1_ref, first_ref, stats_ref, *refs):
    o_refs, (out_ref, tok, cw, w, shifted, conv, whole, stats, more, affine, o, out, sems) = refs[:-13], refs[-13:]
    count, blocks, part, deep = w.shape[0], w.shape[2], w.shape[4], w.shape[5]
    channels = whole.shape[1]
    serial = iter(range(64))

    def load(source, target):
        return pltpu.make_async_copy(source, target, sems.at[next(serial)])

    def start(loads):
        for copy in loads:
            copy.start()

    def wait(loads):
        for copy in loads:
            copy.wait()

    early = [load(tok_ref, tok), load(cw_ref, cw)]
    pieces = [[load(r.at[:, i], w.at[i, m]) for m, r in enumerate((w0_ref, w1_ref))] for i in range(count)]
    middle = [load(first_ref, conv.at[0]), load(stats_ref, stats), load(affine_ref, affine)]
    late = []
    for i, r in enumerate(o_refs):
        m, q = i // len(QUARTERS), i % len(QUARTERS)
        late.append(load(r.at[:, 2] if q == 0 else r, o.at[m, q]))
    start(early + pieces[0])
    wait(early + pieces[0])
    start(sum(pieces[1:], []) + middle)
    for i in range(count):
        if i == 1:
            wait(pieces[1])
            start(late)
        elif i > 1:
            wait(pieces[i])
        piece = w.at[i]
        value, gate = joined(piece, blocks, 0), joined(piece, blocks, 1)
        convolve(i == 0, tok, cw.at[pl.ds(1 + i, 1)], value, gate, conv.at[1 + i], more, shifted)
    wait(middle)
    mean = jnp.sum(stats[0] + more[0], axis=1, keepdims=True) / channels
    meansq = jnp.sum(stats[1] + more[1], axis=1, keepdims=True) / channels
    scale = lax.rsqrt(meansq - mean * mean + EPS)
    for q in range(len(QUARTERS)):
        here = slice(q * part, (q + 1) * part)
        v = (conv[q].astype(jnp.float32) - mean) * scale * affine[0:1, here] + affine[1:2, here]
        whole[:, here] = (v / (1.0 + jnp.exp(-v))).astype(jnp.bfloat16)
    wait(late)
    stores = []
    for x in range(blocks):
        for m in range(2):
            right = jnp.concatenate([o[m, q, x] for q in range(len(QUARTERS))], axis=0)
            at = 2 * x + m
            out[at] = jnp.dot(whole[...], right, preferred_element_type=jnp.float32).astype(jnp.bfloat16)
            stores.append(load(out.at[at], out_ref.at[:, columns(where_ref, x, m, deep)]))
            stores[-1].start()
    wait(stores)


SMEM, VMEM, HBM, ANY = (pl.BlockSpec(memory_space=space) for space in (pltpu.SMEM, pltpu.VMEM, pltpu.HBM, pl.ANY))


def kernel(function, specs, outs, scratch, flops, mib, *operands):
    return pl.pallas_call(
        function,
        out_shape=[o[0] for o in outs],
        in_specs=specs,
        out_specs=[o[1] for o in outs],
        scratch_shapes=scratch,
        compiler_params=pltpu.CompilerParams(vmem_limit_bytes=mib * 1024 * 1024),
        cost_estimate=pl.CostEstimate(flops=flops, bytes_accessed=8 * 1024 * 1024, transcendentals=0),
    )(*operands)


def per_device(tokens, w_value, w_gate, conv_weight, norm_gain, norm_bias, w_out):
    rows = tokens[0]
    length, depth = rows.shape
    taps, channels = conv_weight.shape
    positions = lax.axis_size(("zh", "zl"))
    core, side, parity = (lax.axis_index(a) for a in ("core", "side", "zl"))
    where = jnp.stack([core, side, parity]).astype(jnp.int32)

    both = jnp.stack([w_value.T, w_gate.T, w_out])
    half = both.shape[1] // 2
    mine = lax.dynamic_slice_in_dim(both, side * half, half, 1)
    far = lax.all_gather(mine, "zh", axis=0, tiled=True)
    own = far.reshape(lax.axis_size("zh"), *mine.shape).transpose(1, 0, 2, 3)
    own = own.reshape(3, -1, mine.shape[-1])

    vg = own[:2]
    vg_side = swapped(vg, "side")
    own0 = exchanged(copies(own, "x"), "x")
    vg_zl = swapped(jnp.stack([vg, vg_side]), "zl")
    last = rows[length - HALO :]
    halo = lax.ppermute(last, ("zh", "zl"), [(i, i + 1) for i in range(positions - 1)])
    rest = jnp.concatenate([vg_side[None], vg_zl], axis=0)
    rest0 = exchanged(copies(rest, "x"), "x")
    o00 = own0[:, 2]
    o10 = swapped(o00, "side")
    o01 = swapped(o00, "zl")
    own1 = swapped(own0, "core")
    o11 = swapped(o01, "side")
    o10c = swapped(o10, "core")
    o01c = swapped(o01, "core")
    o11c = swapped(o11, "core")
    rest1 = swapped(rest0, "core")

    shape, vmem, dma = jax.ShapeDtypeStruct, pltpu.VMEM, pltpu.SemaphoreType.DMA
    part, blocks, deep = channels // 4, own0.shape[0], own0.shape[-1]
    tok = ((length + HALO, depth), jnp.bfloat16)
    cw = ((4, taps, part), jnp.float32)
    stats = (shape((2, length, LANES), jnp.float32), VMEM)
    shifted = vmem((8, length + HALO, part), jnp.float32)
    flops = 2 * length * depth * channels // 2
    conv_a, stats_a, tok_ready, cw_ready, affine = kernel(
        first, [SMEM] + [HBM] * 5 + [ANY] * 2,
        [(shape((length, part), jnp.bfloat16), VMEM), stats, (shape(*tok), HBM), (shape(*cw), HBM),
         (shape((8, channels), jnp.float32), HBM)],
        [vmem(*tok), vmem(*cw), vmem((2, blocks, 2, part, deep), jnp.bfloat16), shifted,
         vmem((taps, channels), jnp.bfloat16), vmem((16, channels), jnp.float32),
         vmem((8, channels), jnp.float32), dma((8 + 4 * blocks,))],
        flops, 56, where, halo, rows, conv_weight, norm_gain[None], norm_bias[None], own0, own1,
    )
    (mixed,) = kernel(
        remaining, [SMEM, HBM, HBM, HBM, ANY, ANY, HBM, HBM] + [ANY] * 8,
        [(shape((length, depth), jnp.bfloat16), HBM)],
        [vmem(*tok), vmem(*cw), vmem((3, 2, blocks, 2, part, deep), jnp.bfloat16), shifted,
         vmem((4, length, part), jnp.bfloat16), vmem((length, channels), jnp.bfloat16),
         vmem((2, length, LANES), jnp.float32), vmem((2, length, LANES), jnp.float32),
         vmem((8, channels), jnp.float32), vmem((2, 4, blocks, part, deep), jnp.bfloat16),
         vmem((2 * blocks, length, deep), jnp.bfloat16), dma((32,))],
        3 * flops, 56, where, tok_ready, cw_ready, affine, rest0, rest1, conv_a, stats_a,
        own0, o10, o01, o11, own1, o10c, o01c, o11c,
    )
    return mixed[None]


def solution(mesh):
    groups, positions, columns = (mesh.shape[a] for a in ("grp", "sp", "dp"))
    fine = Mesh(
        mesh.devices.reshape(groups // 2, 2, positions // 2, 2, columns // 2, 2),
        ("pair", "side", "zh", "zl", "x", "core"),
    )
    z, dp = ("zh", "zl"), ("x", "core")
    placed = (
        P(("pair", "side", *dp), z, None),
        P(dp, z),
        P(dp, z),
        P(),
        P(),
        P(),
        P(z, dp),
    )
    return jax.shard_map(
        per_device,
        mesh=fine,
        in_specs=placed,
        out_specs=P(("pair", "side", *dp), z, None),
        check_vma=False,
    )
```

```python
import jax
import jax.numpy as jnp
from jax import lax
from jax.experimental import pallas as pl
from jax.experimental.pallas import tpu as pltpu
from jax.sharding import Mesh, PartitionSpec as P


EPS = 1e-05
HALO = 32
LANES = 128
QUARTERS = ((0, 0), (1, 0), (0, 1), (1, 1))


def copies(block, axis):
    return jnp.broadcast_to(block, (lax.axis_size(axis), *block.shape))


def exchanged(blocks, axis):
    return lax.all_to_all(blocks, axis, 0, 0)


def swapped(array, axis):
    return lax.ppermute(array, axis, [(0, 1), (1, 0)])


def columns(where_ref, x, m, deep):
    core = where_ref[0]
    c = core if m == 0 else 1 - core
    return pl.ds(pl.multiple_of((2 * x + c) * deep, deep), deep)


def chosen(array, where_ref, quarter, precision=None):
    side = where_ref[1] if quarter[0] == 0 else 1 - where_ref[1]
    parity = where_ref[2] if quarter[1] == 0 else 1 - where_ref[2]
    width = LANES // 8
    wide = 4 * LANES
    source = lax.broadcasted_iota(jnp.int32, (wide, LANES), 0)
    target = lax.broadcasted_iota(jnp.int32, (wide, LANES), 1)
    pick = source == (target // width) * (4 * width) + parity * (2 * width) + side * width + target % width
    pick = jnp.where(pick, 1.0, 0.0).astype(array.dtype)
    parts = [array[:, at : at + wide] for at in range(0, array.shape[1], wide)]
    parts = [jnp.dot(p, pick, preferred_element_type=jnp.float32, precision=precision) for p in parts]
    return jnp.concatenate(parts, axis=1)


def convolve(fresh, tok, cw, value, gate, conv_ref, stats_ref, shifted):
    rows, part = conv_ref.shape[0], value.shape[0]
    taps = cw.shape[1]
    nt = (((1,), (1,)), ((), ()))
    value = lax.dot_general(tok[...], value, nt, preferred_element_type=jnp.float32)
    gate = lax.dot_general(tok[...], gate, nt, preferred_element_type=jnp.float32)
    glu = (value * jax.nn.sigmoid(gate)).astype(jnp.bfloat16).astype(jnp.float32)
    shifted[0] = glu
    for r in range(1, 8):
        shifted[r] = pltpu.roll(glu, r, 0)
    half = rows // 2
    for at in range(0, part, LANES):
        here = slice(at, at + LANES)
        for h in range(2):
            acc = jnp.zeros((half, LANES), jnp.float32)
            for k in range(taps):
                r, j = k % 8, k // 8
                begin = HALO - 8 * j + h * half
                acc = acc + cw[0, k : k + 1, here] * shifted[r, begin : begin + half, here]
            acc = acc.astype(jnp.bfloat16)
            when = slice(h * half, (h + 1) * half)
            conv_ref[when, here] = acc
            acc = acc.astype(jnp.float32)
            if fresh and at == 0:
                stats_ref[0, when] = acc
                stats_ref[1, when] = acc * acc
            else:
                stats_ref[0, when] += acc
                stats_ref[1, when] += acc * acc


def joined(w, blocks, *index):
    return jnp.concatenate([w[(m, x, *index)] for x in range(blocks) for m in range(2)], axis=1)


def first(
    where_ref, halo_ref, tok_ref, cw_ref, gain_ref, bias_ref, w0_ref, w1_ref, side0_ref, side1_ref,
    conv_ref, stats_ref, tok_out, cw_out, affine_out,
    tok, cw, w, shifted, taps, raw, affine, sems,
):
    blocks = w.shape[2]
    rows, deep = tok_ref.shape[0], tok.shape[1] // (2 * blocks)
    loads = [pltpu.make_async_copy(cw_ref, taps, sems.at[0])]
    for at in range(2 * blocks):
        here, there = pl.ds(at * deep, deep), columns(where_ref, at // 2, at % 2, deep)
        loads.append(pltpu.make_async_copy(halo_ref.at[:, there], tok.at[pl.ds(0, HALO), here], sems.at[8 + 2 * at]))
        loads.append(pltpu.make_async_copy(tok_ref.at[:, there], tok.at[pl.ds(HALO, rows), here], sems.at[9 + 2 * at]))
    for m, r in enumerate((w0_ref, w1_ref)):
        loads.append(pltpu.make_async_copy(r.at[:, pl.ds(0, 2)], w.at[0, m], sems.at[1 + m]))
    later = [pltpu.make_async_copy(r, w.at[1, m], sems.at[8 + 4 * blocks + m]) for m, r in enumerate((side0_ref, side1_ref))]
    loads.append(pltpu.make_async_copy(gain_ref, raw.at[pl.ds(0, 1)], sems.at[5]))
    loads.append(pltpu.make_async_copy(bias_ref, raw.at[pl.ds(8, 1)], sems.at[6]))
    for load in loads + later:
        load.start()
    loads[0].wait()
    loads[-2].wait()
    loads[-1].wait()
    pair = jnp.concatenate([raw[0:1], raw[8:9], jnp.zeros((6, raw.shape[1]), jnp.float32)], axis=0)
    part = cw.shape[2]
    for i, quarter in enumerate(QUARTERS):
        cw[i] = chosen(taps[...], where_ref, quarter)
        affine[:, i * part : (i + 1) * part] = chosen(pair, where_ref, quarter, lax.Precision.HIGHEST)
    for load in loads[1:-2]:
        load.wait()
    stores = [
        pltpu.make_async_copy(tok, tok_out, sems.at[3]),
        pltpu.make_async_copy(cw, cw_out, sems.at[4]),
        pltpu.make_async_copy(affine, affine_out, sems.at[7]),
    ]
    for store in stores:
        store.start()
    for load in later:
        load.wait()
    for q in range(2):
        piece = w.at[q]
        value, gate = joined(piece, blocks, 0), joined(piece, blocks, 1)
        convolve(q == 0, tok, cw.at[pl.ds(q, 1)], value, gate, conv_ref.at[q], stats_ref, shifted)
    for store in stores:
        store.wait()


def remaining(where_ref, tok_ref, cw_ref, affine_ref, w0_ref, w1_ref, first_ref, stats_ref, *refs):
    o_refs, (out_ref, tok, cw, w, shifted, conv, whole, stats, more, affine, o, out, sems) = refs[:-13], refs[-13:]
    count, blocks, part, deep = w.shape[0], w.shape[2], w.shape[4], w.shape[5]
    channels = whole.shape[1]
    serial = iter(range(64))

    def load(source, target):
        return pltpu.make_async_copy(source, target, sems.at[next(serial)])

    def start(loads):
        for copy in loads:
            copy.start()

    def wait(loads):
        for copy in loads:
            copy.wait()

    early = [load(tok_ref, tok), load(cw_ref, cw)]
    pieces = [[load(r.at[:, i], w.at[i, m]) for m, r in enumerate((w0_ref, w1_ref))] for i in range(count)]
    middle = [load(first_ref, conv.at[pl.ds(0, 2)]), load(stats_ref, stats), load(affine_ref, affine)]
    late = []
    for i, r in enumerate(o_refs):
        m, q = i // len(QUARTERS), i % len(QUARTERS)
        late.append(load(r.at[:, 2] if q == 0 else r, o.at[m, q]))
    start(early + pieces[0])
    wait(early + pieces[0])
    start(sum(pieces[1:], []) + middle)
    for i in range(count):
        if i == 1:
            wait(pieces[1])
            start(late)
        elif i > 1:
            wait(pieces[i])
        piece = w.at[i]
        value, gate = joined(piece, blocks, 0), joined(piece, blocks, 1)
        convolve(i == 0, tok, cw.at[pl.ds(2 + i, 1)], value, gate, conv.at[2 + i], more, shifted)
    wait(middle)
    mean = jnp.sum(stats[0] + more[0], axis=1, keepdims=True) / channels
    meansq = jnp.sum(stats[1] + more[1], axis=1, keepdims=True) / channels
    scale = lax.rsqrt(meansq - mean * mean + EPS)
    for q in range(len(QUARTERS)):
        here = slice(q * part, (q + 1) * part)
        v = (conv[q].astype(jnp.float32) - mean) * scale * affine[0:1, here] + affine[1:2, here]
        whole[:, here] = (v / (1.0 + jnp.exp(-v))).astype(jnp.bfloat16)
    wait(late)
    stores = []
    for x in range(blocks):
        for m in range(2):
            right = jnp.concatenate([o[m, q, x] for q in range(len(QUARTERS))], axis=0)
            at = 2 * x + m
            out[at] = jnp.dot(whole[...], right, preferred_element_type=jnp.float32).astype(jnp.bfloat16)
            stores.append(load(out.at[at], out_ref.at[:, columns(where_ref, x, m, deep)]))
            stores[-1].start()
    wait(stores)


SMEM, VMEM, HBM, ANY = (pl.BlockSpec(memory_space=space) for space in (pltpu.SMEM, pltpu.VMEM, pltpu.HBM, pl.ANY))


def kernel(function, specs, outs, scratch, flops, mib, *operands):
    return pl.pallas_call(
        function,
        out_shape=[o[0] for o in outs],
        in_specs=specs,
        out_specs=[o[1] for o in outs],
        scratch_shapes=scratch,
        compiler_params=pltpu.CompilerParams(vmem_limit_bytes=mib * 1024 * 1024),
        cost_estimate=pl.CostEstimate(flops=flops, bytes_accessed=8 * 1024 * 1024, transcendentals=0),
    )(*operands)


def per_device(tokens, w_value, w_gate, conv_weight, norm_gain, norm_bias, w_out):
    rows = tokens[0]
    length, depth = rows.shape
    taps, channels = conv_weight.shape
    positions = lax.axis_size(("zh", "zl"))
    core, side, parity = (lax.axis_index(a) for a in ("core", "side", "zl"))
    where = jnp.stack([core, side, parity]).astype(jnp.int32)

    both = jnp.stack([w_value.T, w_gate.T, w_out])
    half = both.shape[1] // 2
    mine = lax.dynamic_slice_in_dim(both, side * half, half, 1)
    far = lax.all_gather(mine, "zh", axis=0, tiled=True)
    own = far.reshape(lax.axis_size("zh"), *mine.shape).transpose(1, 0, 2, 3)
    own = own.reshape(3, -1, mine.shape[-1])

    vg = own[:2]
    own0 = exchanged(copies(own, "x"), "x")
    vg_side = swapped(vg, "side")
    vg_zl = swapped(vg, "zl")
    last = rows[length - HALO :]
    halo = lax.ppermute(last, ("zh", "zl"), [(i, i + 1) for i in range(positions - 1)])
    side0 = exchanged(copies(vg_side, "x"), "x")
    vg_both = swapped(vg_zl, "side")
    rest0 = exchanged(copies(jnp.stack([vg_zl, vg_both]), "x"), "x")
    side1 = swapped(side0, "core")
    o00 = own0[:, 2]
    o10 = swapped(o00, "side")
    o01 = swapped(o00, "zl")
    own1 = swapped(own0, "core")
    o11 = swapped(o01, "side")
    o10c = swapped(o10, "core")
    o01c = swapped(o01, "core")
    o11c = swapped(o11, "core")
    rest1 = swapped(rest0, "core")

    shape, vmem, dma = jax.ShapeDtypeStruct, pltpu.VMEM, pltpu.SemaphoreType.DMA
    part, blocks, deep = channels // 4, own0.shape[0], own0.shape[-1]
    tok = ((length + HALO, depth), jnp.bfloat16)
    cw = ((4, taps, part), jnp.float32)
    stats = (shape((2, length, LANES), jnp.float32), VMEM)
    shifted = vmem((8, length + HALO, part), jnp.float32)
    flops = 2 * length * depth * channels // 2
    conv_a, stats_a, tok_ready, cw_ready, affine = kernel(
        first, [SMEM] + [HBM] * 5 + [ANY] * 4,
        [(shape((2, length, part), jnp.bfloat16), VMEM), stats, (shape(*tok), HBM), (shape(*cw), HBM),
         (shape((8, channels), jnp.float32), HBM)],
        [vmem(*tok), vmem(*cw), vmem((2, 2, blocks, 2, part, deep), jnp.bfloat16), shifted,
         vmem((taps, channels), jnp.bfloat16), vmem((16, channels), jnp.float32),
         vmem((8, channels), jnp.float32), dma((10 + 4 * blocks,))],
        flops, 56, where, halo, rows, conv_weight, norm_gain[None], norm_bias[None], own0, own1, side0, side1,
    )
    (mixed,) = kernel(
        remaining, [SMEM, HBM, HBM, HBM, ANY, ANY, HBM, HBM] + [ANY] * 8,
        [(shape((length, depth), jnp.bfloat16), HBM)],
        [vmem(*tok), vmem(*cw), vmem((2, 2, blocks, 2, part, deep), jnp.bfloat16), shifted,
         vmem((4, length, part), jnp.bfloat16), vmem((length, channels), jnp.bfloat16),
         vmem((2, length, LANES), jnp.float32), vmem((2, length, LANES), jnp.float32),
         vmem((8, channels), jnp.float32), vmem((2, 4, blocks, part, deep), jnp.bfloat16),
         vmem((2 * blocks, length, deep), jnp.bfloat16), dma((32,))],
        3 * flops, 56, where, tok_ready, cw_ready, affine, rest0, rest1, conv_a, stats_a,
        own0, o10, o01, o11, own1, o10c, o01c, o11c,
    )
    return mixed[None]


def solution(mesh):
    groups, positions, columns = (mesh.shape[a] for a in ("grp", "sp", "dp"))
    fine = Mesh(
        mesh.devices.reshape(groups // 2, 2, positions // 2, 2, columns // 2, 2),
        ("pair", "side", "zh", "zl", "x", "core"),
    )
    z, dp = ("zh", "zl"), ("x", "core")
    placed = (
        P(("pair", "side", *dp), z, None),
        P(dp, z),
        P(dp, z),
        P(),
        P(),
        P(),
        P(z, dp),
    )
    return jax.shard_map(
        per_device,
        mesh=fine,
        in_specs=placed,
        out_specs=P(("pair", "side", *dp), z, None),
        check_vma=False,
    )
```

```python
import jax
import jax.numpy as jnp
from jax import lax
from jax.experimental import pallas as pl
from jax.experimental.pallas import tpu as pltpu
from jax.sharding import Mesh, PartitionSpec as P


EPS = 1e-05
HALO = 32
LANES = 128
QUARTERS = ((0, 0), (1, 0), (0, 1), (1, 1))


def copies(block, axis):
    return jnp.broadcast_to(block, (lax.axis_size(axis), *block.shape))


def exchanged(blocks, axis):
    return lax.all_to_all(blocks, axis, 0, 0)


def swapped(array, axis):
    return lax.ppermute(array, axis, [(0, 1), (1, 0)])


def columns(where_ref, x, m, deep):
    core = where_ref[0]
    c = core if m == 0 else 1 - core
    return pl.ds(pl.multiple_of((2 * x + c) * deep, deep), deep)


def chosen(array, where_ref, quarter):
    side = where_ref[1] if quarter[0] == 0 else 1 - where_ref[1]
    parity = where_ref[2] if quarter[1] == 0 else 1 - where_ref[2]
    width = LANES // 8
    wide = 4 * LANES
    source = lax.broadcasted_iota(jnp.int32, (wide, LANES), 0)
    target = lax.broadcasted_iota(jnp.int32, (wide, LANES), 1)
    pick = source == (target // width) * (4 * width) + parity * (2 * width) + side * width + target % width
    pick = jnp.where(pick, 1.0, 0.0).astype(array.dtype)
    parts = [array[:, at : at + wide] for at in range(0, array.shape[1], wide)]
    parts = [jnp.dot(p, pick, preferred_element_type=jnp.float32) for p in parts]
    return jnp.concatenate(parts, axis=1)


def convolve(fresh, tok, cw, value, gate, conv_ref, stats_ref, shifted):
    rows, part = conv_ref.shape[0], value.shape[0]
    taps = cw.shape[1]
    nt = (((1,), (1,)), ((), ()))
    value = lax.dot_general(tok[...], value, nt, preferred_element_type=jnp.float32)
    gate = lax.dot_general(tok[...], gate(), nt, preferred_element_type=jnp.float32)
    glu = (value * jax.nn.sigmoid(gate)).astype(jnp.bfloat16).astype(jnp.float32)
    shifted[0] = glu
    for r in range(1, 8):
        shifted[r] = pltpu.roll(glu, r, 0)
    half = rows // 2
    for at in range(0, part, LANES):
        here = slice(at, at + LANES)
        for h in range(2):
            acc = jnp.zeros((half, LANES), jnp.float32)
            for k in range(taps):
                r, j = k % 8, k // 8
                begin = HALO - 8 * j + h * half
                acc = acc + cw[0, k : k + 1, here] * shifted[r, begin : begin + half, here]
            acc = acc.astype(jnp.bfloat16)
            when = slice(h * half, (h + 1) * half)
            conv_ref[when, here] = acc
            acc = acc.astype(jnp.float32)
            if fresh and at == 0:
                stats_ref[0, when] = acc
                stats_ref[1, when] = acc * acc
            else:
                stats_ref[0, when] += acc
                stats_ref[1, when] += acc * acc


def joined(w, blocks, *index):
    return jnp.concatenate([w[(m, x, *index)] for x in range(blocks) for m in range(2)], axis=1)


def first(
    where_ref, halo_ref, tok_ref, cw_ref, gain_ref, bias_ref, w0_ref, w1_ref, conv_ref, stats_ref, tok_out, cw_out, affine_out,
    tok, cw, w, shifted, taps, raw, affine, sems,
):
    blocks = w.shape[1]
    rows, deep = tok_ref.shape[0], tok.shape[1] // (2 * blocks)
    loads = [pltpu.make_async_copy(cw_ref, taps, sems.at[0])]
    for at in range(2 * blocks):
        here, there = pl.ds(at * deep, deep), columns(where_ref, at // 2, at % 2, deep)
        loads.append(pltpu.make_async_copy(halo_ref.at[:, there], tok.at[pl.ds(0, HALO), here], sems.at[8 + 2 * at]))
        loads.append(pltpu.make_async_copy(tok_ref.at[:, there], tok.at[pl.ds(HALO, rows), here], sems.at[9 + 2 * at]))
    for m, r in enumerate((w0_ref, w1_ref)):
        loads.append(pltpu.make_async_copy(r.at[:, pl.ds(0, 2)], w.at[m], sems.at[1 + m]))
    loads.append(pltpu.make_async_copy(gain_ref, raw.at[pl.ds(0, 1)], sems.at[5]))
    loads.append(pltpu.make_async_copy(bias_ref, raw.at[pl.ds(8, 1)], sems.at[6]))
    for load in loads:
        load.start()
    loads[0].wait()
    loads[-2].wait()
    loads[-1].wait()
    pair = jnp.concatenate([raw[0:1], raw[8:9], jnp.zeros((6, raw.shape[1]), jnp.float32)], axis=0)
    high = pair.astype(jnp.bfloat16).astype(jnp.float32)
    middle = (pair - high).astype(jnp.bfloat16).astype(jnp.float32)
    thirds = jnp.concatenate([high, middle, pair - high - middle, jnp.zeros_like(pair)], axis=0).astype(jnp.bfloat16)
    part = cw.shape[2]
    for i, quarter in enumerate(QUARTERS):
        cw[i] = chosen(taps[...], where_ref, quarter)
        third = chosen(thirds, where_ref, quarter)
        affine[:, i * part : (i + 1) * part] = third[0:8] + (third[8:16] + third[16:24])
    for load in loads[1:-2]:
        load.wait()
    stores = [
        pltpu.make_async_copy(tok, tok_out, sems.at[3]),
        pltpu.make_async_copy(cw, cw_out, sems.at[4]),
        pltpu.make_async_copy(affine, affine_out, sems.at[7]),
    ]
    for store in stores:
        store.start()
    convolve(True, tok, cw.at[pl.ds(0, 1)], joined(w, blocks, 0), lambda: joined(w, blocks, 1), conv_ref, stats_ref, shifted)
    for store in stores:
        store.wait()


def remaining(where_ref, tok_ref, cw_ref, affine_ref, w0_ref, w1_ref, first_ref, stats_ref, *refs):
    o_refs, (out_ref, tok, cw, w, shifted, conv, whole, stats, more, affine, o, out, sems) = refs[:-13], refs[-13:]
    count, blocks, part, deep = w.shape[0], w.shape[2], w.shape[4], w.shape[5]
    channels = whole.shape[1]
    serial = iter(range(64))

    def load(source, target):
        return pltpu.make_async_copy(source, target, sems.at[next(serial)])

    def start(loads):
        for copy in loads:
            copy.start()

    def wait(loads):
        for copy in loads:
            copy.wait()

    early = [load(tok_ref, tok), load(cw_ref, cw)]
    pieces = [[load(r.at[:, i], w.at[i, m]) for m, r in enumerate((w0_ref, w1_ref))] if i else [] for i in range(count)]
    middle = [load(first_ref, conv.at[0]), load(stats_ref, stats), load(affine_ref, affine)]
    late = []
    for i, r in enumerate(o_refs):
        m, q = i // len(QUARTERS), i % len(QUARTERS)
        late.append(load(r.at[:, 2] if q == 0 else r, o.at[m, q]))
    head, tail = ([load(r.at[:, 0, k], w.at[0, m, :, k]) for m, r in enumerate((w0_ref, w1_ref))] for k in range(2))
    start(early + head + tail)
    wait(early + head)
    for i in range(count):
        if i == 1:
            wait(pieces[1])
            start(late)
        elif i > 1:
            wait(pieces[i])
        piece = w.at[i]

        def gate(i=i, piece=piece):
            if i == 0:
                wait(tail)
                start(sum(pieces[1:], []) + middle)
            return joined(piece, blocks, 1)

        value = joined(piece, blocks, 0)
        convolve(i == 0, tok, cw.at[pl.ds(1 + i, 1)], value, gate, conv.at[1 + i], more, shifted)
    wait(middle)
    mean = jnp.sum(stats[0] + more[0], axis=1, keepdims=True) / channels
    meansq = jnp.sum(stats[1] + more[1], axis=1, keepdims=True) / channels
    scale = lax.rsqrt(meansq - mean * mean + EPS)
    for q in range(len(QUARTERS)):
        here = slice(q * part, (q + 1) * part)
        v = (conv[q].astype(jnp.float32) - mean) * scale * affine[0:1, here] + affine[1:2, here]
        whole[:, here] = (v / (1.0 + jnp.exp(-v))).astype(jnp.bfloat16)
    wait(late)
    stores = []
    for x in range(blocks):
        for m in range(2):
            right = jnp.concatenate([o[m, q, x] for q in range(len(QUARTERS))], axis=0)
            at = 2 * x + m
            out[at] = jnp.dot(whole[...], right, preferred_element_type=jnp.float32).astype(jnp.bfloat16)
            stores.append(load(out.at[at], out_ref.at[:, columns(where_ref, x, m, deep)]))
            stores[-1].start()
    wait(stores)


SMEM, VMEM, HBM, ANY = (pl.BlockSpec(memory_space=space) for space in (pltpu.SMEM, pltpu.VMEM, pltpu.HBM, pl.ANY))


def kernel(function, specs, outs, scratch, flops, mib, *operands):
    return pl.pallas_call(
        function,
        out_shape=[o[0] for o in outs],
        in_specs=specs,
        out_specs=[o[1] for o in outs],
        scratch_shapes=scratch,
        compiler_params=pltpu.CompilerParams(vmem_limit_bytes=mib * 1024 * 1024),
        cost_estimate=pl.CostEstimate(flops=flops, bytes_accessed=8 * 1024 * 1024, transcendentals=0),
    )(*operands)


def per_device(tokens, w_value, w_gate, conv_weight, norm_gain, norm_bias, w_out):
    rows = tokens[0]
    length, depth = rows.shape
    taps, channels = conv_weight.shape
    positions = lax.axis_size(("zh", "zl"))
    core, side, parity = (lax.axis_index(a) for a in ("core", "side", "zl"))
    where = jnp.stack([core, side, parity]).astype(jnp.int32)

    both = jnp.stack([w_value.T, w_gate.T, w_out])
    half = both.shape[1] // 2
    mine = lax.dynamic_slice_in_dim(both, side * half, half, 1)
    far = lax.all_gather(mine, "zh", axis=0, tiled=True)
    own = far.reshape(lax.axis_size("zh"), *mine.shape).transpose(1, 0, 2, 3)
    own = own.reshape(3, -1, mine.shape[-1])

    vg = own[:2]
    vg_side = swapped(vg, "side")
    own0 = exchanged(copies(own, "x"), "x")
    vg_zl = swapped(jnp.stack([vg, vg_side]), "zl")
    last = rows[length - HALO :]
    halo = lax.ppermute(last, ("zh", "zl"), [(i, i + 1) for i in range(positions - 1)])
    rest = jnp.concatenate([vg_side[None], vg_zl], axis=0)
    rest0 = exchanged(copies(rest, "x"), "x")
    o00 = own0[:, 2]
    o10 = swapped(o00, "side")
    o01 = swapped(o00, "zl")
    own1 = swapped(own0, "core")
    o11 = swapped(o01, "side")
    o10c = swapped(o10, "core")
    o01c = swapped(o01, "core")
    o11c = swapped(o11, "core")
    rest1 = swapped(rest0, "core")

    shape, vmem, dma = jax.ShapeDtypeStruct, pltpu.VMEM, pltpu.SemaphoreType.DMA
    part, blocks, deep = channels // 4, own0.shape[0], own0.shape[-1]
    tok = ((length + HALO, depth), jnp.bfloat16)
    cw = ((4, taps, part), jnp.float32)
    stats = (shape((2, length, LANES), jnp.float32), VMEM)
    shifted = vmem((8, length + HALO, part), jnp.float32)
    flops = 2 * length * depth * channels // 2
    conv_a, stats_a, tok_ready, cw_ready, affine = kernel(
        first, [SMEM] + [HBM] * 5 + [ANY] * 2,
        [(shape((length, part), jnp.bfloat16), VMEM), stats, (shape(*tok), HBM), (shape(*cw), HBM),
         (shape((8, channels), jnp.float32), HBM)],
        [vmem(*tok), vmem(*cw), vmem((2, blocks, 2, part, deep), jnp.bfloat16), shifted,
         vmem((taps, channels), jnp.bfloat16), vmem((16, channels), jnp.float32),
         vmem((8, channels), jnp.float32), dma((8 + 4 * blocks,))],
        flops, 56, where, halo, rows, conv_weight, norm_gain[None], norm_bias[None], own0, own1,
    )
    (mixed,) = kernel(
        remaining, [SMEM, HBM, HBM, HBM, ANY, ANY, HBM, HBM] + [ANY] * 8,
        [(shape((length, depth), jnp.bfloat16), HBM)],
        [vmem(*tok), vmem(*cw), vmem((3, 2, blocks, 2, part, deep), jnp.bfloat16), shifted,
         vmem((4, length, part), jnp.bfloat16), vmem((length, channels), jnp.bfloat16),
         vmem((2, length, LANES), jnp.float32), vmem((2, length, LANES), jnp.float32),
         vmem((8, channels), jnp.float32), vmem((2, 4, blocks, part, deep), jnp.bfloat16),
         vmem((2 * blocks, length, deep), jnp.bfloat16), dma((32,))],
        3 * flops, 56, where, tok_ready, cw_ready, affine, rest0, rest1, conv_a, stats_a,
        own0, o10, o01, o11, own1, o10c, o01c, o11c,
    )
    return mixed[None]


def solution(mesh):
    groups, positions, columns = (mesh.shape[a] for a in ("grp", "sp", "dp"))
    fine = Mesh(
        mesh.devices.reshape(groups // 2, 2, positions // 2, 2, columns // 2, 2),
        ("pair", "side", "zh", "zl", "x", "core"),
    )
    z, dp = ("zh", "zl"), ("x", "core")
    placed = (
        P(("pair", "side", *dp), z, None),
        P(dp, z),
        P(dp, z),
        P(),
        P(),
        P(),
        P(z, dp),
    )
    return jax.shard_map(
        per_device,
        mesh=fine,
        in_specs=placed,
        out_specs=P(("pair", "side", *dp), z, None),
        check_vma=False,
    )
```
